256 devices in a mesh: grp: 2 (over y), sp: 32 (over z, core), tp: 4 (over x).
Axes of the slice: x: 4, y: 2, z: 16, core: 2. Of those that a mesh axis runs over, the one named last changes fastest.
The devices are a block of a 4x16x16 slice.
Arguments:
- residual: bfloat16 [16384, 2048], P(('grp', 'sp', 'tp')), parts along dimension 0, may hold values from -6 to 6
- query_nope: bfloat16 [16384, 1024], P(('grp', 'sp'), 'tp'), parts along dimension 0, may hold values from -6 to 6
- query_rope: bfloat16 [16384, 512], P(('grp', 'sp'), 'tp'), parts along dimension 0, may hold values from -240 to 240
- kv_latent: bfloat16 [16384, 256], P(('grp', 'sp')), parts along dimension 0, may hold values from -6 to 6
- rope_key: bfloat16 [16384, 64], P(('grp', 'sp')), parts along dimension 0, may hold values from -6 to 6
- latent_gain: float32 [256], replicated, may hold values from 0.1 to 1.9
- w_key: bfloat16 [256, 1024], P(None, 'tp'), may hold values from -0.375 to 0.375
- w_value: bfloat16 [256, 1024], P(None, 'tp'), may hold values from -0.375 to 0.375
- w_out: bfloat16 [1024, 2048], P('tp'), may hold values from -0.1875 to 0.1875
- post_gain: float32 [2048], replicated, may hold values from 0.1 to 1.9
- routes: int32 [16384, 2], P(('grp', 'sp', 'tp')), parts along dimension 0, may hold values from 0 to 31, all different within a row; in each aligned block of 64 rows (0 to 63, 64 to 127, ...) at most 6 rows name the same one
- route_weight: float32 [16384, 2], P(('grp', 'sp', 'tp')), parts along dimension 0, may hold values from 0.25 to 1
- moe_gain: float32 [2048], replicated, may hold values from 0.1 to 1.9
- w_gate: bfloat16 [32, 2048, 3584], P('sp', None, 'tp'), may hold values from -0.125 to 0.125
- w_up: bfloat16 [32, 2048, 3584], P('sp', None, 'tp'), may hold values from -0.125 to 0.125
- w_down: bfloat16 [32, 3584, 2048], P('sp', 'tp'), may hold values from -0.09375 to 0.09375
Outputs:
- mixed: bfloat16 [16384, 2048], P(('grp', 'sp', 'tp')), parts along dimension 0
The draws below stay inside these ranges and needn't reach their ends.
There are 2 independent parts, one for each index of `grp`. The reference program is written for one: setup_inputs(seed, part) draws one part's arguments, and reference() takes and returns one part's arrays. A program takes and returns all parts, laid end to end along the dimension named above; an argument that names none is the same for every part. Nothing has to cross between parts.
Inputs may be any that keep to these rules, and one draw needn't show every extreme that they name: `routes`: each row names two different experts. Among the 64 rows of one device no expert is named more than 6 times, and some device names some expert exactly 6 times.
All inputs are finite; a program needn't handle non-finite values.
Results may differ from the reference program's by a relative error of at most 0.014.
Values may be sent and summed in bfloat16 or wider, within the bound.
A program may use at most 128 MiB of HBM per device.

```python
import math
import jax
import jax.numpy as jnp
import numpy as np
from jax import lax

D = 2048
HEADS = 8
NOPE = 128
ROPE = 64
VDIM = 128
KV_RANK = 256
FF = 3584
SEQ = 8192
TOK_DEV = 64
EXPERTS = 32
CAP = 6
N_SP = 32
N_TP = 4


def draw_query_rope(key, part):
    shape = (SEQ, HEADS * ROPE)
    values = jax.random.normal(jax.random.fold_in(key, 11), shape, jnp.float32)
    return jnp.clip(values, -240.0, 240.0).astype(jnp.bfloat16)


def block_scale(own_key, dims, split, least, high):
    gain = 1.0
    for dim, parts in split:
        steps = jax.random.uniform(jax.random.fold_in(jax.random.fold_in(own_key, 6), dim), (parts,), jnp.float32, least / len(split), high / len(split))
        gain = gain * jnp.repeat(jnp.exp(steps), dims[dim] // parts).reshape((-1,) + (1,) * (len(dims) - 1 - dim))
    return gain


def assign_block(key, own, number, rows, number_of, top, reach, lean):
    order = jax.random.permutation(key, number_of)
    heavy_load, ordinary = load_shares(number_of, rows * top, reach, lean, True), load_shares(number_of, rows * top, reach, lean, False)
    places = jnp.arange(number_of)

    def named(lengths, offset_by):
        used = int((lengths > 0).sum())
        fixed = max(1, used // 4)
        moved = fixed + (places - fixed + offset_by * (used - fixed)) % max(1, number_of - fixed)
        return jnp.zeros((number_of,), jnp.int32).at[order[jnp.where(places < fixed, places, moved)]].set(jnp.asarray(lengths, jnp.int32))

    lengths = jnp.where(number % 4 == 0, named(heavy_load, number // 4), named(ordinary, number - number // 4 - 1))
    mixed = jax.random.permutation(jax.random.fold_in(own, 3), number_of)
    giver, receiver = mixed[0:number_of // 2 * 2:2], mixed[1:number_of // 2 * 2:2]
    room = jnp.minimum(lengths[giver] - 1, reach - lengths[receiver]) // 2
    room = jnp.where((giver == order[0]) | (receiver == order[0]) | (lengths[receiver] == 0), 0, jnp.maximum(room, 0))
    moved = jax.random.randint(jax.random.fold_in(own, 4), (number_of // 2,), 0, 1 << 20) % (room + 1)
    lengths = lengths.at[giver].add(-moved).at[receiver].add(moved)
    items = jnp.searchsorted(jnp.cumsum(lengths), jnp.arange(rows * top), side="right").astype(jnp.int32)
    table = items.reshape(top, rows).T
    table = table[jax.random.permutation(jax.random.fold_in(own, 1), rows)]
    offset_by = jax.random.randint(jax.random.fold_in(own, 2), (rows, 1), 0, top)
    return jnp.take_along_axis(table, (jnp.arange(top)[None, :] + offset_by) % top, axis=1)


def load_shares(count, total, bound, lean, full):
    loads = [(1 << 20) // math.isqrt(grade ** lean) + 1 for grade in range(1, count + 1)]
    largest = bound if full else min(bound, max(-(-total // count), total * loads[0] // sum(loads)))
    least = 1 if total - largest >= count - 1 else 0
    given, rest = [largest] + [least] * (count - 1), total - largest - least * (count - 1)
    while rest > 0:
        movable = [i for i in range(1, count) if given[i] < largest] or [i for i in range(1, count) if given[i] < bound]
        pool, budget = sum([loads[i] for i in movable]), rest
        for i in movable:
            addition = min(bound - given[i], max(1, budget * loads[i] // pool), rest)
            given[i] = given[i] + addition
            rest = rest - addition
    return np.array(given)


def normal_values(stream_key, dims, width, limit, cuts=(), kind=jnp.bfloat16):
    factor_of = block_scale(stream_key, dims, cuts, -0.22, 0.18) if cuts else 1.0
    drawn = jax.random.normal(stream_key, dims, jnp.float32) * width * factor_of
    return jnp.minimum(jnp.maximum(drawn, -limit), limit).astype(kind)


def setup_inputs(seed: int = 0, part: int = 0) -> dict:
    splits = jax.random.split(jax.random.key(seed), 17)
    part_splits = jax.random.split(jax.random.fold_in(splits[16], part), 17)
    residual = normal_values(part_splits[0], (SEQ, D), 1.0, 6.0, ((0, 128),))
    query_nope = normal_values(part_splits[1], (SEQ, HEADS * NOPE), 1.0, 6.0, ((0, 32), (1, 4)))
    query_rope = draw_query_rope(jax.random.fold_in(jax.random.fold_in(splits[16], part), 71), part)
    kv_latent = normal_values(part_splits[3], (SEQ, KV_RANK), 1.0, 6.0, ((0, 32),))
    rope_key = normal_values(part_splits[4], (SEQ, ROPE), 1.0, 6.0, ((0, 32),))
    latent_gain = jnp.clip(1.0 + 0.18 * jax.random.normal(splits[5], (KV_RANK,), jnp.float32), 0.1, 1.9)
    w_key = normal_values(splits[6], (KV_RANK, HEADS * NOPE), KV_RANK ** -0.5, 0.375, ((1, 4),))
    w_value = normal_values(splits[7], (KV_RANK, HEADS * VDIM), KV_RANK ** -0.5, 0.375, ((1, 4),))
    w_out = normal_values(splits[8], (HEADS * VDIM, D), (HEADS * VDIM) ** -0.5, 0.1875, ((0, 4),))
    post_gain = jnp.clip(1.0 + 0.18 * jax.random.normal(splits[9], (D,), jnp.float32), 0.1, 1.9)
    routes_keys = jax.random.split(jax.random.fold_in(part_splits[10], 1), SEQ // TOK_DEV)
    routes_turns = jax.random.permutation(jax.random.fold_in(part_splits[10], 3), SEQ // TOK_DEV)
    routes = jax.vmap(lambda own, number: assign_block(jax.random.fold_in(part_splits[10], 2), own, number, TOK_DEV, EXPERTS, 2, CAP, 2))(routes_keys, routes_turns).reshape((SEQ, 2))
    route_weight = jnp.clip(0.25 + 0.75 * jax.random.uniform(part_splits[11], (SEQ, 2), jnp.float32) ** block_scale(part_splits[11], (SEQ, 2), ((0, 128),), -0.2, 0.2), 0.25, 1.0)
    moe_gain = jnp.clip(1.0 + 0.18 * jax.random.normal(splits[12], (D,), jnp.float32), 0.1, 1.9)
    w_gate = normal_values(splits[13], (EXPERTS, D, FF), D ** -0.5, 0.125, ((0, 32), (2, 4)))
    w_up = normal_values(splits[14], (EXPERTS, D, FF), D ** -0.5, 0.125, ((0, 32), (2, 4)))
    w_down = normal_values(splits[15], (EXPERTS, FF, D), FF ** -0.5, 0.09375, ((0, 32), (1, 4)))
    return dict(residual=residual, query_nope=query_nope, query_rope=query_rope, kv_latent=kv_latent, rope_key=rope_key, latent_gain=latent_gain, w_key=w_key, w_value=w_value, w_out=w_out, post_gain=post_gain, routes=routes, route_weight=route_weight, moe_gain=moe_gain, w_gate=w_gate, w_up=w_up, w_down=w_down)


epsilon = 1e-06
rope_base = 10000.0

def rms_scale(inputs, gain_vector):
    mean_square = lax.optimization_barrier(jnp.mean(inputs * inputs, axis=-1, keepdims=True))
    return inputs * lax.rsqrt(mean_square + epsilon) * gain_vector.astype(jnp.float32)

def tables(positions, rot_width):
    frequency = 1.0 / rope_base ** (jnp.arange(0, rot_width, 2, dtype=jnp.float32) / rot_width)
    angles = positions.astype(jnp.float32)[:, None] * frequency[None, :]
    return (jnp.cos(angles), jnp.sin(angles))

def rotate(inputs, cosine_table, sine_table):
    half_width = inputs.shape[-1] // 2
    first_half = inputs[..., :half_width]
    second_half = inputs[..., half_width:]
    return jnp.concatenate([first_half * cosine_table - second_half * sine_table, second_half * cosine_table + first_half * sine_table], axis=-1)

def reference(residual, query_nope, query_rope, kv_latent, rope_key, latent_gain, w_key, w_value, w_out, post_gain, routes, route_weight, moe_gain, w_gate, w_up, w_down):
    seq_len = residual.shape[0]
    positions = jnp.arange(seq_len, dtype=jnp.int32)
    cosine_table, sine_table = tables(positions, ROPE)
    normed = rms_scale(kv_latent.astype(jnp.float32), latent_gain).astype(jnp.bfloat16)
    key_plain = jnp.dot(normed, w_key, preferred_element_type=jnp.float32).astype(jnp.bfloat16)
    value_plain = jnp.dot(normed, w_value, preferred_element_type=jnp.float32).astype(jnp.bfloat16)
    key_heads = key_plain.reshape(seq_len, HEADS, NOPE).astype(jnp.float32)
    value_heads = value_plain.reshape(seq_len, HEADS, VDIM).astype(jnp.float32)
    key_turned = rotate(rope_key.astype(jnp.float32), cosine_table, sine_table).astype(jnp.bfloat16).astype(jnp.float32)
    query_plain = query_nope.reshape(seq_len, HEADS, NOPE)
    query_turned = rotate(query_rope.reshape(seq_len, HEADS, ROPE).astype(jnp.float32), cosine_table[:, None, :], sine_table[:, None, :]).astype(jnp.bfloat16)
    score_scale = (NOPE + ROPE) ** (-0.5)
    block_len = math.gcd(seq_len, 512)

    def one_block(block_index):
        block_begin = block_index * block_len
        query_block = lax.dynamic_slice_in_dim(query_plain, block_begin, block_len, 0).astype(jnp.float32)
        turned_block = lax.dynamic_slice_in_dim(query_turned, block_begin, block_len, 0).astype(jnp.float32)
        scores = jnp.einsum('thd,shd->hts', query_block, key_heads)
        scores = (scores + jnp.einsum('thd,sd->hts', turned_block, key_turned)) * score_scale
        query_pos = block_begin + jnp.arange(block_len, dtype=jnp.int32)
        allowed = positions[None, :] <= query_pos[:, None]
        scores = jnp.where(allowed[None], scores, -jnp.inf)
        row_max = lax.optimization_barrier(jnp.max(scores, axis=-1, keepdims=True))
        expo = jnp.exp(scores - row_max)
        row_sum = lax.optimization_barrier(jnp.sum(expo, axis=-1))
        probs = lax.optimization_barrier(expo.astype(jnp.bfloat16)).astype(jnp.float32)
        weighted = jnp.einsum('hts,shd->htd', probs, value_heads) / row_sum[..., None]
        return weighted.transpose(1, 0, 2).reshape(block_len, HEADS * VDIM).astype(jnp.bfloat16)
    attended = lax.map(one_block, jnp.arange(seq_len // block_len, dtype=jnp.int32)).reshape(seq_len, HEADS * VDIM)
    group_rows = HEADS * VDIM // N_TP
    branch = jnp.zeros((seq_len, D), jnp.float32)
    for group_id in range(N_TP):
        partial_value = jnp.dot(attended[:, group_id * group_rows:(group_id + 1) * group_rows], w_out[group_id * group_rows:(group_id + 1) * group_rows], preferred_element_type=jnp.float32).astype(jnp.bfloat16)
        branch = branch + lax.optimization_barrier(partial_value).astype(jnp.float32)
    updated = (residual.astype(jnp.float32) + rms_scale(branch, post_gain)).astype(jnp.bfloat16)
    moe_in = rms_scale(updated.astype(jnp.float32), moe_gain).astype(jnp.bfloat16)
    flat_routes = routes.reshape(-1)
    flat_weight = route_weight.reshape(-1).astype(jnp.float32)
    token_ids = jnp.arange(flat_routes.shape[0], dtype=jnp.int32) // 2
    slot_bound = N_SP * N_TP * CAP
    group_width = FF // N_TP

    def one_expert(summed, inputs):
        gate_matrix, up_matrix, down_matrix, expert_id = inputs
        matches = flat_routes == expert_id
        found, = jnp.nonzero(matches, size=slot_bound, fill_value=0)
        filled = (jnp.arange(slot_bound, dtype=jnp.int32) < jnp.sum(matches.astype(jnp.int32))).astype(jnp.float32)
        picked = moe_in[token_ids[found]]
        gate_pre = jnp.dot(picked, gate_matrix, preferred_element_type=jnp.float32)
        up_proj = jnp.dot(picked, up_matrix, preferred_element_type=jnp.float32)
        activated = (jax.nn.silu(gate_pre) * up_proj).astype(jnp.bfloat16)
        grouped = activated.reshape(slot_bound, N_TP, group_width).transpose(1, 0, 2).astype(jnp.float32)
        down_groups = down_matrix.reshape(N_TP, group_width, D).astype(jnp.float32)
        partials = jnp.einsum('gra,gad->grd', grouped, down_groups).astype(jnp.bfloat16)
        partials = lax.optimization_barrier(partials)
        expert_out = lax.optimization_barrier(lax.optimization_barrier(jnp.sum(partials.astype(jnp.float32), axis=0)).astype(jnp.bfloat16))
        scaled = expert_out.astype(jnp.float32) * (flat_weight[found] * filled)[:, None]
        summed = summed.at[token_ids[found]].add(scaled)
        return (summed, None)
    summed, _ = lax.scan(one_expert, jnp.zeros((seq_len, D), jnp.float32), (w_gate, w_up, w_down, jnp.arange(EXPERTS, dtype=jnp.int32)))
    return (updated.astype(jnp.float32) + summed).astype(jnp.bfloat16)
```

```python
import functools

import jax
import jax.numpy as jnp
import numpy as np
from jax import lax
from jax.experimental import pallas as pl
from jax.experimental.pallas import tpu as pltpu
from jax.sharding import PartitionSpec as P

MESH = pl.DeviceIdType.MESH
BF = jnp.bfloat16
F32 = jnp.float32
epsilon = 1e-06
GROUPS = 4
QUARTERS = 4


def remote(src, dst, send_sem, recv_sem, device):
    return pltpu.make_async_remote_copy(
        src_ref=src, dst_ref=dst, send_sem=send_sem, recv_sem=recv_sem,
        device_id=device, device_id_type=MESH,
    )


def rms_scale(inputs, gain_vector):
    mean_square = jnp.mean(inputs * inputs, axis=-1, keepdims=True)
    return inputs * lax.rsqrt(mean_square + epsilon) * gain_vector


def dot(a, b, dims=((1,), (0,))):
    return lax.dot_general(a, b, (dims, ((), ())), preferred_element_type=F32)


def moe_kernel(
    n_sp, n_tp, cap,
    updated_ref, routes_ref, weight_ref, gain_ref, fold_ref, unfold_ref, wg_hbm, wu_hbm, wd_hbm,
    out_ref,
    wg, wu, wd, spots, send, recv, rows_in, hidden, partial, opposite, joined, arrived, back, returned,
    w_sem, zs, zr, xs, xr, ys, yr, rs, rr,
):
    n_z = n_sp // 2
    sp, tp = lax.axis_index("sp"), lax.axis_index("tp")
    z, core = lax.div(sp, 2), lax.rem(sp, 2)
    right, left = lax.rem(tp + 1, n_tp), lax.rem(tp + n_tp - 1, n_tp)
    tok, width = updated_ref.shape
    part = width // QUARTERS
    half = width // 2
    block = cap * QUARTERS
    per = n_z // GROUPS
    own_rows = per * 2 * cap

    loads = [
        pltpu.make_async_copy(src.at[0], dst, w_sem.at[i])
        for i, (src, dst) in enumerate(((wg_hbm, wg), (wu_hbm, wu), (wd_hbm, wd)))
    ]
    for load in loads:
        load.start()

    barrier = pltpu.get_barrier_semaphore()

    def greet(i, carry):
        pl.semaphore_signal(barrier, inc=1, device_id={"sp": lax.rem(sp + i, n_sp)}, device_id_type=MESH)
        return carry

    lax.fori_loop(1, n_sp, greet, 0)
    for i in range(1, n_tp):
        pl.semaphore_signal(barrier, inc=1, device_id={"tp": lax.rem(tp + i, n_tp)}, device_id_type=MESH)

    updated = updated_ref[...].astype(F32)
    moe_in = rms_scale(updated, gain_ref[...]).astype(BF)
    stacked = jnp.concatenate([moe_in[:, q * part:(q + 1) * part] for q in range(QUARTERS)], axis=0)

    expert_ids = lax.broadcasted_iota(jnp.int32, (tok, n_sp), 1)
    chosen = [routes_ref[:, k:k + 1] for k in range(2)]
    hits = [(chosen[k] == expert_ids).astype(F32) for k in range(2)]
    earlier = (
        lax.broadcasted_iota(jnp.int32, (tok, tok), 1) < lax.broadcasted_iota(jnp.int32, (tok, tok), 0)
    ).astype(F32).astype(BF)
    order = dot(earlier, (hits[0] + hits[1]).astype(BF))
    slots = lax.broadcasted_iota(jnp.int32, (tok, n_sp * block), 1)
    for k in range(2):
        place = jnp.sum(order * hits[k], axis=1, keepdims=True).astype(jnp.int32)
        ahead = (lax.shift_right_logical(chosen[k], 1) - z + n_z) & (n_z - 1)
        turn = jnp.where(ahead < n_z // 2, n_z - 1 - 2 * ahead, 2 * ahead - n_z)
        first = (2 * turn + (chosen[k] & 1)) * block + place
        for q in range(QUARTERS):
            spots[k, q * tok:(q + 1) * tok, :] = (slots == first + q * cap).astype(F32).astype(BF)
    sending = dot(spots[0] + spots[1], stacked, ((0,), (0,)))
    for i in range(n_sp):
        send[i // 2, i % 2] = sending[i * block:(i + 1) * block].astype(BF)

    pl.semaphore_wait(barrier, n_sp - 1 + n_tp - 1)

    def ahead_of(k):
        return jnp.where(lax.rem(k, 2) == 1, lax.div(n_z - 1 - k, 2), lax.div(n_z + k, 2))

    def dispatch_copy(k, to_core):
        target = lax.rem(z + ahead_of(k), n_z) * 2 + to_core
        return remote(send.at[k, to_core], recv.at[k, core], zs.at[k, to_core], zr.at[k, core], {"sp": target})

    def dispatch_arrival(k, from_core):
        return remote(send.at[k, from_core], recv.at[k, from_core], zs.at[k, from_core], zr.at[k, from_core], {"sp": sp})

    def return_copy(k, to_core):
        target = lax.rem(z - ahead_of(k) + n_z, n_z) * 2 + to_core
        return remote(back.at[k, to_core], returned.at[k, core], rs.at[k, to_core], rr.at[k, core], {"sp": target})

    def return_arrival(k, from_core):
        return remote(back.at[k, from_core], returned.at[k, from_core], rs.at[k, from_core], rr.at[k, from_core], {"sp": sp})

    last = n_z - 1

    def start_dispatch(k, carry):
        for to_core in range(2):
            @pl.when(jnp.logical_or(k < last, core != to_core))
            def _():
                dispatch_copy(k, to_core).start()
        return carry

    lax.fori_loop(0, n_z, start_dispatch, 0)
    recv[last, core] = send[last, core]

    def to_right(src, dst, ss, rr_, i, j):
        return remote(src, dst, ss.at[i, j], rr_.at[i, j], {"tp": right})

    def to_left(src, dst, ss, rr_, i, j):
        return remote(src, dst, ss.at[i, j], rr_.at[i, j], {"tp": left})

    low, high = pl.ds(0, half), pl.ds(half, half)

    def gather_copies(g):
        return (
            to_right(rows_in.at[g, 0], rows_in.at[g, 1], xs, xr, g, 0),
            to_left(rows_in.at[g, 0], rows_in.at[g, 2], xs, xr, g, 1),
            to_right(rows_in.at[g, 1, :, low], rows_in.at[g, 3, :, low], xs, xr, g, 2),
            to_left(rows_in.at[g, 2, :, high], rows_in.at[g, 3, :, high], xs, xr, g, 3),
        )

    def reduce_copies(g):
        return (
            to_right(partial.at[g, 3, :, low], opposite.at[g, 0], ys, yr, g, 0),
            to_left(partial.at[g, 3, :, high], opposite.at[g, 1], ys, yr, g, 1),
            to_right(partial.at[g, 2, :, high], arrived.at[g, 0, :, high], ys, yr, g, 2),
            to_left(partial.at[g, 1, :, low], arrived.at[g, 1, :, low], ys, yr, g, 3),
            to_right(joined.at[g, 0], arrived.at[g, 0, :, low], ys, yr, g, 4),
            to_left(joined.at[g, 1], arrived.at[g, 1, :, high], ys, yr, g, 5),
        )

    def collect(g):
        for i in range(per):
            for from_core in range(2):
                k = g * per + i

                @pl.when(jnp.logical_or(k < last, core != from_core))
                def _():
                    dispatch_arrival(k, from_core).wait_recv()
        raw = recv[pl.ds(g * per, per)].reshape(per * 2 * block, part)
        rows = dot(fold_ref[...], raw).astype(BF)
        for q in range(QUARTERS):
            rows_in[g, 0, :, q * part:(q + 1) * part] = rows[q * own_rows:(q + 1) * own_rows]
        copies = gather_copies(g)
        copies[0].start()
        copies[1].start()

    def pass_on(g):
        copies = gather_copies(g)
        copies[0].wait_recv()
        copies[2].start()
        copies[1].wait_recv()
        copies[3].start()

    def experts(g):
        @pl.when(g == 0)
        def _():
            for load in loads:
                load.wait()

        copies = gather_copies(g)
        copies[2].wait_recv()
        copies[3].wait_recv()
        rows = rows_in[g].reshape(n_tp * own_rows, width)
        gate = dot(rows, wg[...])
        up = dot(rows, wu[...])
        hidden[...] = (gate / (1.0 + jnp.exp(-gate)) * up).astype(BF)
        step = 512
        for n in range(width // step):
            down = dot(hidden[...], wd[:, n * step:(n + 1) * step]).astype(BF)
            partial[g, :, :, n * step:(n + 1) * step] = down.reshape(n_tp, own_rows, step)
        for copy in reduce_copies(g)[:4]:
            copy.start()

    def add_opposite(g):
        copies = reduce_copies(g)
        copies[0].wait_recv()
        joined[g, 0] = (partial[g, 2, :, :half].astype(F32) + opposite[g, 0].astype(F32)).astype(BF)
        copies[4].start()
        copies[1].wait_recv()
        joined[g, 1] = (partial[g, 1, :, half:].astype(F32) + opposite[g, 1].astype(F32)).astype(BF)
        copies[5].start()

    def give_back(g):
        for copy in reduce_copies(g)[2:]:
            copy.wait_recv()
        total = (
            partial[g, 0].astype(F32) + arrived[g, 0].astype(F32) + arrived[g, 1].astype(F32)
        ).astype(BF)
        stack = jnp.concatenate([total[:, q * part:(q + 1) * part] for q in range(QUARTERS)], axis=0)
        blocks = dot(unfold_ref[...], stack)
        for i in range(2 * per):
            back[g * per + i // 2, i % 2] = blocks[i * block:(i + 1) * block].astype(BF)
        for i in range(per):
            for to_core in range(2):
                k = g * per + i

                @pl.when(jnp.logical_or(k < last, core != to_core))
                def _():
                    return_copy(k, to_core).start()

    def step(g, carry):
        @pl.when(g < GROUPS)
        def _():
            collect(g)

        @pl.when(g > 0)
        def _():
            add_opposite(g - 1)

        @pl.when(g < GROUPS)
        def _():
            pass_on(g)

        @pl.when(g > 0)
        def _():
            give_back(g - 1)

        @pl.when(g < GROUPS)
        def _():
            experts(g)

        return carry

    lax.fori_loop(0, GROUPS + 1, step, 0)
    returned[last, core] = back[last, core]

    def finish_turn(k, carry):
        for other in range(2):
            @pl.when(jnp.logical_or(k < last, core != other))
            def _():
                dispatch_copy(k, other).wait_send()
                return_copy(k, other).wait_send()
                return_arrival(k, other).wait_recv()
        return carry

    lax.fori_loop(0, n_z, finish_turn, 0)

    def finish_group(g, carry):
        for copy in gather_copies(g) + reduce_copies(g):
            copy.wait_send()
        return carry

    lax.fori_loop(0, GROUPS, finish_group, 0)

    outs = returned[...].reshape(n_sp * block, part)
    first = dot(spots[0], outs)
    second = dot(spots[1], outs)
    for q in range(QUARTERS):
        columns = pl.ds(q * part, part)
        near = slice(q * tok, (q + 1) * tok)
        out_ref[:, columns] = (
            updated_ref[:, columns].astype(F32)
            + first[near] * weight_ref[:, 0:1]
            + second[near] * weight_ref[:, 1:2]
        ).astype(BF)


def fold_matrices(sources, cap):
    rows = sources * cap * QUARTERS
    fold = np.zeros((rows, rows), np.float32)
    for q in range(QUARTERS):
        for source in range(sources):
            for slot in range(cap):
                fold[(q * sources + source) * cap + slot, (source * QUARTERS + q) * cap + slot] = 1.0
    return jnp.asarray(fold, BF), jnp.asarray(fold.T, BF)


def moe(updated, routes, route_weight, moe_gain, w_gate, w_up, w_down):
    n_sp, n_tp = lax.axis_size("sp"), lax.axis_size("tp")
    tok, width = updated.shape
    ff = w_gate.shape[2]
    cap = max(2, 3 * tok // n_sp)
    n_z = n_sp // 2
    block, part, half = cap * QUARTERS, width // QUARTERS, width // 2
    per = n_z // GROUPS
    own = per * 2 * cap
    fold, unfold = fold_matrices(per * 2, cap)
    vmem = pl.BlockSpec(memory_space=pltpu.VMEM)
    hbm = pl.BlockSpec(memory_space=pl.ANY)
    dma = pltpu.SemaphoreType.DMA
    return pl.pallas_call(
        functools.partial(moe_kernel, n_sp, n_tp, cap),
        out_shape=jax.ShapeDtypeStruct((tok, width), BF),
        in_specs=[vmem] * 6 + [hbm] * 3,
        out_specs=vmem,
        scratch_shapes=[
            pltpu.VMEM((width, ff), BF),
            pltpu.VMEM((width, ff), BF),
            pltpu.VMEM((ff, width), BF),
            pltpu.VMEM((2, QUARTERS * tok, n_sp * block), BF),
            pltpu.VMEM((n_z, 2, block, part), BF),
            pltpu.VMEM((n_z, 2, block, part), BF),
            pltpu.VMEM((GROUPS, n_tp, own, width), BF),
            pltpu.VMEM((n_tp * own, ff), BF),
            pltpu.VMEM((GROUPS, n_tp, own, width), BF),
            pltpu.VMEM((GROUPS, 2, own, half), BF),
            pltpu.VMEM((GROUPS, 2, own, half), BF),
            pltpu.VMEM((GROUPS, 2, own, width), BF),
            pltpu.VMEM((n_z, 2, block, part), BF),
            pltpu.VMEM((n_z, 2, block, part), BF),
            dma((3,)),
            dma((n_z, 2)), dma((n_z, 2)),
            dma((GROUPS, 4)), dma((GROUPS, 4)),
            dma((GROUPS, 6)), dma((GROUPS, 6)),
            dma((n_z, 2)), dma((n_z, 2)),
        ],
        compiler_params=pltpu.CompilerParams(
            collective_id=1, has_side_effects=True, vmem_limit_bytes=60 * 1024 * 1024
        ),
    )(updated, routes, route_weight, moe_gain.reshape(1, -1), fold, unfold, w_gate, w_up, w_down)


HEADS = 8
NOPE = 128
ROPE = 64
VDIM = 128
SP = "sp"
GRP_SP_TP = ("grp", "sp", "tp")
GRP_SP = ("grp", "sp")


rope_base = 10000.0


def side_by_side(arrays, axis, dim, along):
    widths = [a.shape[along] for a in arrays]
    both = jnp.concatenate(arrays, axis=along)
    result = lax.all_gather(both, axis, axis=dim, tiled=True)
    return tuple(jnp.split(result, [sum(widths[:k]) for k in range(1, len(widths))], axis=along))


def split_up(array, dim, length):
    before, after = (array.shape[:dim], array.shape[dim + 1 :])
    return jnp.moveaxis(array.reshape(*before, length, -1, *after), dim, 0)


def summed_on_arrival(array, axis, dim):
    length = lax.axis_size(axis)
    pieces = lax.all_to_all(split_up(array, dim, length), axis, 0, 0, tiled=True)
    return jnp.sum(pieces.astype(jnp.float32), axis=0)


def tables(positions, rot_width):
    frequency = 1.0 / rope_base ** (jnp.arange(0, rot_width, 2, dtype=jnp.float32) / rot_width)
    angles = positions.astype(jnp.float32)[:, None] * frequency[None, :]
    return (jnp.cos(angles), jnp.sin(angles))


def rotate(inputs, cosine_table, sine_table):
    half_width = inputs.shape[-1] // 2
    first_half = inputs[..., :half_width]
    second_half = inputs[..., half_width:]
    return jnp.concatenate(
        [
            first_half * cosine_table - second_half * sine_table,
            second_half * cosine_table + first_half * sine_table,
        ],
        axis=-1,
    )


def expand(latent_rows, rope_rows, latent_gain, w_key, w_value):
    normed = rms_scale(latent_rows.astype(jnp.float32), latent_gain).astype(jnp.bfloat16)
    key_plain = jnp.dot(normed, w_key, preferred_element_type=jnp.float32).astype(jnp.bfloat16)
    value_plain = jnp.dot(normed, w_value, preferred_element_type=jnp.float32).astype(jnp.bfloat16)
    key_positions = jnp.arange(latent_rows.shape[0], dtype=jnp.int32)
    cosine_table, sine_table = tables(key_positions, rope_rows.shape[1])
    key_turned = rotate(rope_rows.astype(jnp.float32), cosine_table, sine_table).astype(
        jnp.bfloat16
    )
    return (key_plain, value_plain, key_turned)


def body(
    residual,
    query_nope,
    query_rope,
    kv_latent,
    rope_key,
    latent_gain,
    w_key,
    w_value,
    w_out,
    post_gain,
    routes,
    route_weight,
    moe_gain,
    w_gate,
    w_up,
    w_down,
):
    tok_rows = query_nope.shape[0]
    heads_here = HEADS // lax.axis_size("tp")
    first_row = lax.axis_index(SP) * tok_rows
    last_row = first_row + tok_rows - 1
    positions = first_row + jnp.arange(tok_rows, dtype=jnp.int32)
    cosine_table, sine_table = tables(positions, ROPE)
    query_plain = query_nope.reshape(tok_rows, heads_here, NOPE)
    query_turned = rotate(
        query_rope.reshape(tok_rows, heads_here, ROPE).astype(jnp.float32),
        cosine_table[:, None, :],
        sine_table[:, None, :],
    ).astype(jnp.bfloat16)
    score_scale = (NOPE + ROPE) ** (-0.5)

    def update(state_now, key_plain, value_plain, key_turned):
        row_max, row_sum, running = state_now
        key_count = key_plain.shape[0]
        key_heads = key_plain.reshape(key_count, heads_here, NOPE)
        value_heads = value_plain.reshape(key_count, heads_here, VDIM)
        scores = jnp.einsum(
            "thd,shd->hts", query_plain, key_heads, preferred_element_type=jnp.float32
        )
        scores = (
            scores
            + jnp.einsum(
                "thd,sd->hts", query_turned, key_turned, preferred_element_type=jnp.float32
            )
        ) * score_scale
        key_positions = jnp.arange(key_count, dtype=jnp.int32)
        allowed = key_positions[None, :] <= positions[:, None]
        scores = jnp.where(allowed[None], scores, -1e30)
        new_max = jnp.maximum(row_max, jnp.max(scores, axis=-1))
        weights = jnp.exp(scores - new_max[..., None])
        row_sum = jnp.sum(weights, axis=-1)
        running = jnp.einsum(
            "hts,shd->htd",
            weights.astype(jnp.bfloat16),
            value_heads,
            preferred_element_type=jnp.float32,
        )
        return (new_max, row_sum, running)

    start_state = (
        jnp.full((heads_here, tok_rows), -1e30, jnp.float32),
        jnp.zeros((heads_here, tok_rows), jnp.float32),
        jnp.zeros((heads_here, tok_rows, VDIM), jnp.float32),
    )
    pieces = side_by_side((kv_latent, rope_key), SP, 0, 1)

    def take_piece(state_in):
        key_plain, value_plain, key_turned = expand(
            pieces[0], pieces[1], latent_gain, w_key, w_value
        )
        return update(state_in, key_plain, value_plain, key_turned)

    def skip_piece(state_in):
        return state_in

    final_state = lax.cond(jnp.int32(0) <= last_row, take_piece, skip_piece, start_state)
    attended = (final_state[2] / final_state[1][..., None]).transpose(1, 0, 2)
    attended = attended.reshape(tok_rows, heads_here * VDIM).astype(jnp.bfloat16)
    chosen = attended
    product = jnp.dot(chosen, w_out, preferred_element_type=jnp.float32)
    branch = summed_on_arrival(
        product.astype(jnp.bfloat16).astype(jnp.float32).astype(jnp.bfloat16), "tp", 0
    )
    updated = (residual.astype(jnp.float32) + rms_scale(branch, post_gain)).astype(jnp.bfloat16)
    return moe(updated, routes, route_weight, moe_gain, w_gate, w_up, w_down)


def solution(mesh):
    placed = (
        P(GRP_SP_TP, None),
        P(GRP_SP, "tp"),
        P(GRP_SP, "tp"),
        P(GRP_SP, None),
        P(GRP_SP, None),
        P(),
        P(None, "tp"),
        P(None, "tp"),
        P("tp", None),
        P(),
        P(GRP_SP_TP, None),
        P(GRP_SP_TP, None),
        P(),
        P(SP, None, "tp"),
        P(SP, None, "tp"),
        P(SP, "tp", None),
    )
    return jax.shard_map(
        body, mesh=mesh, in_specs=placed, out_specs=P(GRP_SP_TP, None), check_vma=False
    )
```

```python
import functools

import jax
import jax.numpy as jnp
import numpy as np
from jax import lax
from jax.experimental import pallas as pl
from jax.experimental.pallas import tpu as pltpu
from jax.sharding import PartitionSpec as P

MESH = pl.DeviceIdType.MESH
BF = jnp.bfloat16
F32 = jnp.float32
epsilon = 1e-06
rope_base = 10000.0
SP = "sp"
GRP_SP_TP = ("grp", "sp", "tp")
GRP_SP = ("grp", "sp")
GROUPS = 4
QUARTERS = 4


def remote(src, dst, send_sem, recv_sem, device):
    return pltpu.make_async_remote_copy(
        src_ref=src, dst_ref=dst, send_sem=send_sem, recv_sem=recv_sem,
        device_id=device, device_id_type=MESH,
    )


def rms_scale(inputs, gain_vector):
    mean_square = jnp.mean(inputs * inputs, axis=-1, keepdims=True)
    return inputs * lax.rsqrt(mean_square + epsilon) * gain_vector


def dot(a, b, dims=((1,), (0,))):
    return lax.dot_general(a, b, (dims, ((), ())), preferred_element_type=F32)


def moe_kernel(
    n_sp, n_tp, cap,
    updated_ref, routes_ref, weight_ref, gain_ref, fold_ref, unfold_ref, wg_hbm, wu_hbm, wd_hbm,
    out_ref,
    wg, wu, wd, spots, send, recv, rows_in, hidden, partial, opposite, joined, arrived, back, returned,
    w_sem, zs, zr, xs, xr, ys, yr, rs, rr,
):
    n_z = n_sp // 2
    sp, tp = lax.axis_index("sp"), lax.axis_index("tp")
    z, core = lax.div(sp, 2), lax.rem(sp, 2)
    right, left = lax.rem(tp + 1, n_tp), lax.rem(tp + n_tp - 1, n_tp)
    tok, width = updated_ref.shape
    part = width // QUARTERS
    half = width // 2
    block = cap * QUARTERS
    per = n_z // GROUPS
    own_rows = per * 2 * cap

    loads = [
        pltpu.make_async_copy(src.at[0], dst, w_sem.at[i])
        for i, (src, dst) in enumerate(((wg_hbm, wg), (wu_hbm, wu), (wd_hbm, wd)))
    ]
    for load in loads:
        load.start()

    barrier = pltpu.get_barrier_semaphore()

    def greet(i, carry):
        pl.semaphore_signal(barrier, inc=1, device_id={"sp": lax.rem(sp + i, n_sp)}, device_id_type=MESH)
        return carry

    lax.fori_loop(1, n_sp, greet, 0)
    for i in range(1, n_tp):
        pl.semaphore_signal(barrier, inc=1, device_id={"tp": lax.rem(tp + i, n_tp)}, device_id_type=MESH)

    updated = updated_ref[...].astype(F32)
    moe_in = rms_scale(updated, gain_ref[...]).astype(BF)
    stacked = jnp.concatenate([moe_in[:, q * part:(q + 1) * part] for q in range(QUARTERS)], axis=0)

    expert_ids = lax.broadcasted_iota(jnp.int32, (tok, n_sp), 1)
    chosen = [routes_ref[:, k:k + 1] for k in range(2)]
    hits = [(chosen[k] == expert_ids).astype(F32) for k in range(2)]
    earlier = (
        lax.broadcasted_iota(jnp.int32, (tok, tok), 1) < lax.broadcasted_iota(jnp.int32, (tok, tok), 0)
    ).astype(F32).astype(BF)
    order = dot(earlier, (hits[0] + hits[1]).astype(BF))
    slots = lax.broadcasted_iota(jnp.int32, (tok, n_sp * block), 1)
    for k in range(2):
        place = jnp.sum(order * hits[k], axis=1, keepdims=True).astype(jnp.int32)
        ahead = (lax.shift_right_logical(chosen[k], 1) - z + n_z) & (n_z - 1)
        turn = jnp.where(ahead < n_z // 2, n_z - 1 - 2 * ahead, 2 * ahead - n_z)
        first = (2 * turn + (chosen[k] & 1)) * block + place
        for q in range(QUARTERS):
            spots[k, q * tok:(q + 1) * tok, :] = (slots == first + q * cap).astype(F32).astype(BF)
    sending = dot(spots[0] + spots[1], stacked, ((0,), (0,)))
    for i in range(n_sp):
        send[i // 2, i % 2] = sending[i * block:(i + 1) * block].astype(BF)

    pl.semaphore_wait(barrier, n_sp - 1 + n_tp - 1)

    def ahead_of(k):
        return jnp.where(lax.rem(k, 2) == 1, lax.div(n_z - 1 - k, 2), lax.div(n_z + k, 2))

    def dispatch_copy(k, to_core):
        target = lax.rem(z + ahead_of(k), n_z) * 2 + to_core
        return remote(send.at[k, to_core], recv.at[k, core], zs.at[k, to_core], zr.at[k, core], {"sp": target})

    def dispatch_arrival(k, from_core):
        return remote(send.at[k, from_core], recv.at[k, from_core], zs.at[k, from_core], zr.at[k, from_core], {"sp": sp})

    def return_copy(k, to_core):
        target = lax.rem(z - ahead_of(k) + n_z, n_z) * 2 + to_core
        return remote(back.at[k, to_core], returned.at[k, core], rs.at[k, to_core], rr.at[k, core], {"sp": target})

    def return_arrival(k, from_core):
        return remote(back.at[k, from_core], returned.at[k, from_core], rs.at[k, from_core], rr.at[k, from_core], {"sp": sp})

    last = n_z - 1

    def start_dispatch(k, carry):
        for to_core in range(2):
            @pl.when(jnp.logical_or(k < last, core != to_core))
            def _():
                dispatch_copy(k, to_core).start()
        return carry

    lax.fori_loop(0, n_z, start_dispatch, 0)
    recv[last, core] = send[last, core]

    def to_right(src, dst, ss, rr_, i, j):
        return remote(src, dst, ss.at[i, j], rr_.at[i, j], {"tp": right})

    def to_left(src, dst, ss, rr_, i, j):
        return remote(src, dst, ss.at[i, j], rr_.at[i, j], {"tp": left})

    low, high = pl.ds(0, half), pl.ds(half, half)

    def gather_copies(g):
        return (
            to_right(rows_in.at[g, 0], rows_in.at[g, 1], xs, xr, g, 0),
            to_left(rows_in.at[g, 0], rows_in.at[g, 2], xs, xr, g, 1),
            to_right(rows_in.at[g, 1, :, low], rows_in.at[g, 3, :, low], xs, xr, g, 2),
            to_left(rows_in.at[g, 2, :, high], rows_in.at[g, 3, :, high], xs, xr, g, 3),
        )

    def reduce_copies(g):
        return (
            to_right(partial.at[g, 3, :, low], opposite.at[g, 0], ys, yr, g, 0),
            to_left(partial.at[g, 3, :, high], opposite.at[g, 1], ys, yr, g, 1),
            to_right(partial.at[g, 2, :, high], arrived.at[g, 0, :, high], ys, yr, g, 2),
            to_left(partial.at[g, 1, :, low], arrived.at[g, 1, :, low], ys, yr, g, 3),
            to_right(joined.at[g, 0], arrived.at[g, 0, :, low], ys, yr, g, 4),
            to_left(joined.at[g, 1], arrived.at[g, 1, :, high], ys, yr, g, 5),
        )

    def collect(g):
        for i in range(per):
            for from_core in range(2):
                k = g * per + i

                @pl.when(jnp.logical_or(k < last, core != from_core))
                def _():
                    dispatch_arrival(k, from_core).wait_recv()
        raw = recv[pl.ds(g * per, per)].reshape(per * 2 * block, part)
        rows = dot(fold_ref[...], raw).astype(BF)
        for q in range(QUARTERS):
            rows_in[g, 0, :, q * part:(q + 1) * part] = rows[q * own_rows:(q + 1) * own_rows]
        copies = gather_copies(g)
        copies[0].start()
        copies[1].start()

    def pass_on(g):
        copies = gather_copies(g)
        copies[0].wait_recv()
        copies[2].start()
        copies[1].wait_recv()
        copies[3].start()

    def experts(g):
        @pl.when(g == 0)
        def _():
            for load in loads:
                load.wait()

        copies = gather_copies(g)
        copies[2].wait_recv()
        copies[3].wait_recv()
        rows = rows_in[g].reshape(n_tp * own_rows, width)
        gate = dot(rows, wg[...])
        up = dot(rows, wu[...])
        hidden[...] = (gate / (1.0 + jnp.exp(-gate)) * up).astype(BF)
        step = 512
        for n in range(width // step):
            down = dot(hidden[...], wd[:, n * step:(n + 1) * step]).astype(BF)
            partial[g, :, :, n * step:(n + 1) * step] = down.reshape(n_tp, own_rows, step)
        for copy in reduce_copies(g)[:4]:
            copy.start()

    def add_opposite(g):
        copies = reduce_copies(g)
        copies[0].wait_recv()
        joined[g, 0] = (partial[g, 2, :, :half].astype(F32) + opposite[g, 0].astype(F32)).astype(BF)
        copies[4].start()
        copies[1].wait_recv()
        joined[g, 1] = (partial[g, 1, :, half:].astype(F32) + opposite[g, 1].astype(F32)).astype(BF)
        copies[5].start()

    def give_back(g):
        for copy in reduce_copies(g)[2:]:
            copy.wait_recv()
        total = (
            partial[g, 0].astype(F32) + arrived[g, 0].astype(F32) + arrived[g, 1].astype(F32)
        ).astype(BF)
        stack = jnp.concatenate([total[:, q * part:(q + 1) * part] for q in range(QUARTERS)], axis=0)
        blocks = dot(unfold_ref[...], stack)
        for i in range(2 * per):
            back[g * per + i // 2, i % 2] = blocks[i * block:(i + 1) * block].astype(BF)
        for i in range(per):
            for to_core in range(2):
                k = g * per + i

                @pl.when(jnp.logical_or(k < last, core != to_core))
                def _():
                    return_copy(k, to_core).start()

    def step(g, carry):
        @pl.when(g < GROUPS)
        def _():
            collect(g)

        @pl.when(g > 0)
        def _():
            add_opposite(g - 1)

        @pl.when(g < GROUPS)
        def _():
            pass_on(g)

        @pl.when(g > 0)
        def _():
            give_back(g - 1)

        @pl.when(g < GROUPS)
        def _():
            experts(g)

        return carry

    lax.fori_loop(0, GROUPS + 1, step, 0)
    returned[last, core] = back[last, core]

    def finish_turn(k, carry):
        for other in range(2):
            @pl.when(jnp.logical_or(k < last, core != other))
            def _():
                dispatch_copy(k, other).wait_send()
                return_copy(k, other).wait_send()
                return_arrival(k, other).wait_recv()
        return carry

    lax.fori_loop(0, n_z, finish_turn, 0)

    def finish_group(g, carry):
        for copy in gather_copies(g) + reduce_copies(g):
            copy.wait_send()
        return carry

    lax.fori_loop(0, GROUPS, finish_group, 0)

    outs = returned[...].reshape(n_sp * block, part)
    first = dot(spots[0], outs)
    second = dot(spots[1], outs)
    for q in range(QUARTERS):
        columns = pl.ds(q * part, part)
        near = slice(q * tok, (q + 1) * tok)
        out_ref[:, columns] = (
            updated_ref[:, columns].astype(F32)
            + first[near] * weight_ref[:, 0:1]
            + second[near] * weight_ref[:, 1:2]
        ).astype(BF)


def fold_matrices(sources, cap):
    rows = sources * cap * QUARTERS
    fold = np.zeros((rows, rows), np.float32)
    for q in range(QUARTERS):
        for source in range(sources):
            for slot in range(cap):
                fold[(q * sources + source) * cap + slot, (source * QUARTERS + q) * cap + slot] = 1.0
    return jnp.asarray(fold, BF), jnp.asarray(fold.T, BF)


def moe(updated, routes, route_weight, moe_gain, w_gate, w_up, w_down):
    n_sp, n_tp = lax.axis_size("sp"), lax.axis_size("tp")
    tok, width = updated.shape
    ff = w_gate.shape[2]
    cap = max(2, 3 * tok // n_sp)
    n_z = n_sp // 2
    block, part, half = cap * QUARTERS, width // QUARTERS, width // 2
    per = n_z // GROUPS
    own = per * 2 * cap
    fold, unfold = fold_matrices(per * 2, cap)
    vmem = pl.BlockSpec(memory_space=pltpu.VMEM)
    hbm = pl.BlockSpec(memory_space=pl.ANY)
    dma = pltpu.SemaphoreType.DMA
    return pl.pallas_call(
        functools.partial(moe_kernel, n_sp, n_tp, cap),
        out_shape=jax.ShapeDtypeStruct((tok, width), BF),
        in_specs=[vmem] * 6 + [hbm] * 3,
        out_specs=vmem,
        scratch_shapes=[
            pltpu.VMEM((width, ff), BF),
            pltpu.VMEM((width, ff), BF),
            pltpu.VMEM((ff, width), BF),
            pltpu.VMEM((2, QUARTERS * tok, n_sp * block), BF),
            pltpu.VMEM((n_z, 2, block, part), BF),
            pltpu.VMEM((n_z, 2, block, part), BF),
            pltpu.VMEM((GROUPS, n_tp, own, width), BF),
            pltpu.VMEM((n_tp * own, ff), BF),
            pltpu.VMEM((GROUPS, n_tp, own, width), BF),
            pltpu.VMEM((GROUPS, 2, own, half), BF),
            pltpu.VMEM((GROUPS, 2, own, half), BF),
            pltpu.VMEM((GROUPS, 2, own, width), BF),
            pltpu.VMEM((n_z, 2, block, part), BF),
            pltpu.VMEM((n_z, 2, block, part), BF),
            dma((3,)),
            dma((n_z, 2)), dma((n_z, 2)),
            dma((GROUPS, 4)), dma((GROUPS, 4)),
            dma((GROUPS, 6)), dma((GROUPS, 6)),
            dma((n_z, 2)), dma((n_z, 2)),
        ],
        compiler_params=pltpu.CompilerParams(
            collective_id=1, has_side_effects=True, vmem_limit_bytes=60 * 1024 * 1024
        ),
    )(updated, routes, route_weight, moe_gain.reshape(1, -1), fold, unfold, w_gate, w_up, w_down)


def attention_kernel(
    n_sp, n_tp, heads,
    residual_ref, nope_ref, rope_ref, latent_ref, rope_key_ref, latent_gain_ref, cosine_ref, sine_ref,
    w_key_ref, w_value_ref, w_out_ref, post_gain_ref,
    updated_ref,
    kv, q_send, q_recv, queries, top, total, running, values, outs,
    ring_s, ring_r, side_s, side_r, q_s, q_r, w_s, w_r, p_s, p_r,
):
    n_z = n_sp // 2
    sp, tp = lax.axis_index("sp"), lax.axis_index("tp")
    z, core = lax.div(sp, 2), lax.rem(sp, 2)
    right, left = lax.rem(tp + 1, n_tp), lax.rem(tp + n_tp - 1, n_tp)
    rows, rank = latent_ref.shape
    rot = rope_key_ref.shape[1]
    nope = w_key_ref.shape[1] // heads
    tok, width = residual_ref.shape
    packs = rank // rot
    span = rows // packs
    block = rows + span
    partner = {"sp": z * 2 + 1 - core}
    up_chip = {"sp": lax.rem(z + 1, n_z) * 2 + core}
    down_chip = {"sp": lax.rem(z + n_z - 1, n_z) * 2 + core}

    barrier = pltpu.get_barrier_semaphore()
    for device in (partner, up_chip, down_chip):
        pl.semaphore_signal(barrier, inc=1, device_id=device, device_id_type=MESH)
    for i in range(1, n_tp):
        pl.semaphore_signal(barrier, inc=1, device_id={"tp": lax.rem(tp + i, n_tp)}, device_id_type=MESH)

    def rotate(values, cosine, sine):
        half = rot // 2
        lane = lax.broadcasted_iota(jnp.int32, values.shape, 1)
        wide = values.shape[1]
        other = jnp.where(
            (lane & half) == 0, pltpu.roll(values, wide - half, 1), pltpu.roll(values, half, 1)
        )
        return (values * cosine + other * sine).astype(BF)

    normed = rms_scale(latent_ref[...].astype(F32), latent_gain_ref[...]).astype(BF)
    kv[z, core, :rows] = normed
    key_pair = jnp.concatenate([rope_key_ref[...]] * 2, axis=1).astype(F32)
    key_turned = rotate(key_pair, cosine_ref[...], sine_ref[...])[:, :rot]
    kv[z, core, rows:] = jnp.concatenate(
        [key_turned[i * span:(i + 1) * span] for i in range(packs)], axis=1
    )

    pl.semaphore_wait(barrier, 2 + 1 + n_tp - 1)

    cut = block // 2

    def ring_copy(way, s, h):
        chip = lax.rem(z - s + n_z, n_z) if way == 0 else lax.rem(z + s, n_z)
        place = kv.at[chip, core, pl.ds(h * cut, cut)]
        return remote(place, place, ring_s.at[way, s, h], ring_r.at[way, s, h], up_chip if way == 0 else down_chip)

    def source_chip(way, s):
        return lax.rem(z - 1 - s + n_z, n_z) if way == 0 else lax.rem(z + 1 + s, n_z)

    def side_copy(way, s):
        place = kv.at[source_chip(way, s), core]
        return remote(place, place, side_s.at[way, s], side_r.at[way, s], partner)

    far = n_z // 2
    reach = (far, far - 1)
    for h in range(2):
        for way in range(2):
            ring_copy(way, 0, h).start()
    own = kv.at[z, core]
    own_side = remote(own, own, side_s.at[1, far - 1], side_r.at[1, far - 1], partner)
    own_side.start()

    turned = rotate(rope_ref[...].astype(F32), cosine_ref[...], sine_ref[...])
    for h in range(heads):
        columns = slice(h * nope, (h + 1) * nope)
        folded = dot(nope_ref[:, columns], w_key_ref[:, columns], ((1,), (1,))).astype(BF)
        for i in range(n_tp):
            q_send[i, :, h * rank:(h + 1) * rank] = folded[i * tok:(i + 1) * tok]
    for i in range(n_tp):
        q_send[i, :, heads * rank:] = turned[i * tok:(i + 1) * tok]

    def q_copy(i):
        to = lax.rem(tp + i, n_tp)
        return remote(q_send.at[to], q_recv.at[i - 1], q_s.at[i - 1], q_r.at[i - 1], {"tp": to})

    for i in (2, 1, 3):
        q_copy(i).start()

    shares = ((w_value_ref, values), (w_out_ref, outs))

    def share_copies(a):
        own_ref, whole = shares[a]
        deep, wide = own_ref.shape
        mine = pl.ds(core * (deep // 2), deep // 2)
        low, high = pl.ds(0, wide // 2), pl.ds(wide // 2, wide // 2)
        across = (
            remote(own_ref.at[mine], whole.at[0, mine], w_s.at[a, 0], w_r.at[a, 0], {"tp": right}),
            remote(own_ref.at[mine], whole.at[1, mine], w_s.at[a, 1], w_r.at[a, 1], {"tp": left}),
            remote(whole.at[0, mine, low], whole.at[2, mine, low], w_s.at[a, 2], w_r.at[a, 2], {"tp": right}),
            remote(whole.at[1, mine, high], whole.at[2, mine, high], w_s.at[a, 3], w_r.at[a, 3], {"tp": left}),
        )
        beside = tuple(
            remote(whole.at[i, mine], whole.at[i, mine], p_s.at[a, i], p_r.at[a, i], partner) for i in range(3)
        )
        return across, beside

    for a in range(2):
        across, _ = share_copies(a)
        across[0].start()
        across[1].start()

    def place_query(slot, sent):
        for h in range(heads):
            at = (slot * heads + h) * tok
            queries[at:at + tok, :rank] = sent[:, h * rank:(h + 1) * rank]
            queries[at:at + tok, rank:] = sent[:, heads * rank + h * rot:heads * rank + (h + 1) * rot]

    place_query(0, q_send[tp])
    top[...] = jnp.full(top.shape, -1e30, F32)
    total[...] = jnp.zeros(total.shape, F32)
    running[...] = jnp.zeros(running.shape, F32)
    for i in (1, 3, 2):
        q_copy(i).wait_recv()
        place_query(i, q_recv[i - 1])

    scale = (nope + rot) ** (-0.5) * 1.4426950408889634
    lanes = total.shape[1]

    def update(chip, masked):
        latents = kv[chip, :, :rows].reshape(2 * rows, rank)
        packed = kv[chip, :, rows:]
        keys_turned = jnp.concatenate(
            [packed[c, :, i * rot:(i + 1) * rot] for c in range(2) for i in range(packs)], axis=0
        )
        keys = jnp.concatenate([latents, keys_turned], axis=1)
        scores = dot(queries[...], keys, ((1,), (1,))) * scale
        if masked:
            key_at = lax.broadcasted_iota(jnp.int32, scores.shape, 1)
            row_at = (lax.broadcasted_iota(jnp.int32, scores.shape, 0) & (tok - 1)) + core * rows + tp * tok
            scores = jnp.where(key_at <= row_at, scores, -1e30)
        old = top[...]
        new = jnp.maximum(old, jnp.max(scores, axis=1, keepdims=True))
        shrink = jnp.exp2(old - new)
        expo = jnp.exp2(scores - new)
        added = expo[:, :lanes]
        for i in range(1, 2 * rows // lanes):
            added = added + expo[:, i * lanes:(i + 1) * lanes]
        total[...] = total[...] * shrink + added
        running[...] = running[...] * shrink + dot(expo.astype(BF), latents)
        top[...] = new

    own_side.wait_recv()
    update(z, True)

    def pass_half(s, h):
        for way in range(2):
            @pl.when(s < reach[way])
            def _():
                ring_copy(way, s, h).wait_recv()

            @pl.when(s + 1 < reach[way])
            def _():
                ring_copy(way, s + 1, h).start()

    def visit(way, s):
        @pl.when(jnp.logical_and(s >= 0, s < reach[way]))
        def _():
            side_copy(way, s).wait_recv()

            @pl.when(source_chip(way, s) < z)
            def _():
                update(source_chip(way, s), False)

    def ring_step(s, carry):
        pass_half(s, 0)
        visit(0, s - 1)
        pass_half(s, 1)
        for way in range(2):
            @pl.when(s < reach[way])
            def _():
                side_copy(way, s).start()
        visit(1, s - 1)

        @pl.when(s == far - 3)
        def _():
            for a in range(2):
                across, beside = share_copies(a)
                across[0].wait_recv()
                across[2].start()
                beside[0].start()
                across[1].wait_recv()
                across[3].start()
                beside[1].start()

        return carry

    lax.fori_loop(0, far + 1, ring_step, 0)

    for a in range(2):
        across, beside = share_copies(a)
        across[2].wait_recv()
        across[3].wait_recv()
        beside[2].start()

    row_sum = jnp.sum(total[...], axis=1, keepdims=True)
    mixed_latent = (running[...] / row_sum).astype(BF)
    for a in range(2):
        _, beside = share_copies(a)
        for copy in beside:
            copy.wait_recv()

    branch = jnp.zeros((tok, width), F32)
    for slot, kept in enumerate((None, 0, 2, 1)):
        w_value = w_value_ref[...] if kept is None else values[kept]
        w_out = w_out_ref[...] if kept is None else outs[kept]
        attended = []
        for h in range(heads):
            at = (slot * heads + h) * tok
            attended.append(dot(mixed_latent[at:at + tok], w_value[:, h * nope:(h + 1) * nope]).astype(BF))
        branch = branch + dot(jnp.concatenate(attended, axis=1), w_out).astype(BF).astype(F32)
    updated_ref[...] = (
        residual_ref[...].astype(F32) + rms_scale(branch, post_gain_ref[...])
    ).astype(BF)

    def drain(s, carry):
        for way in range(2):
            @pl.when(s < reach[way])
            def _():
                for h in range(2):
                    ring_copy(way, s, h).wait_send()
                side_copy(way, s).wait_send()
        return carry

    lax.fori_loop(0, far, drain, 0)
    own_side.wait_send()
    for i in range(1, n_tp):
        q_copy(i).wait_send()
    for a in range(2):
        across, beside = share_copies(a)
        for copy in across + beside:
            copy.wait_send()


def attention(
    residual, query_nope, query_rope, kv_latent, rope_key, latent_gain, w_key, w_value, w_out, post_gain
):
    n_sp, n_tp = lax.axis_size("sp"), lax.axis_size("tp")
    tok, width = residual.shape
    rows, rank = kv_latent.shape
    rot = rope_key.shape[1]
    heads = query_rope.shape[1] // rot
    n_z = n_sp // 2
    far = n_z // 2
    positions = lax.axis_index("sp") * rows + jnp.arange(rows, dtype=jnp.int32)
    cosine, sine = tables(positions, rot)
    cosine = jnp.concatenate([cosine] * (2 * heads), axis=1)
    sine = jnp.concatenate([-sine, sine] * heads, axis=1)
    block = rows + rot * rows // rank
    span = heads * rank + heads * rot
    vmem = pl.BlockSpec(memory_space=pltpu.VMEM)
    dma = pltpu.SemaphoreType.DMA
    return pl.pallas_call(
        functools.partial(attention_kernel, n_sp, n_tp, heads),
        out_shape=jax.ShapeDtypeStruct((tok, width), BF),
        in_specs=[vmem] * 12,
        out_specs=vmem,
        scratch_shapes=[
            pltpu.VMEM((n_z, 2, block, rank), BF),
            pltpu.VMEM((n_tp, tok, span), BF),
            pltpu.VMEM((n_tp - 1, tok, span), BF),
            pltpu.VMEM((n_tp * heads * tok, rank + rot), BF),
            pltpu.VMEM((n_tp * heads * tok, 1), F32),
            pltpu.VMEM((n_tp * heads * tok, 128), F32),
            pltpu.VMEM((n_tp * heads * tok, rank), F32),
            pltpu.VMEM((n_tp - 1,) + w_value.shape, BF),
            pltpu.VMEM((n_tp - 1,) + w_out.shape, BF),
            dma((2, far, 2)), dma((2, far, 2)),
            dma((2, far)), dma((2, far)),
            dma((n_tp - 1,)), dma((n_tp - 1,)),
            dma((2, 4)), dma((2, 4)),
            dma((2, 3)), dma((2, 3)),
        ],
        compiler_params=pltpu.CompilerParams(
            collective_id=0, has_side_effects=True, vmem_limit_bytes=60 * 1024 * 1024
        ),
    )(
        residual, query_nope, query_rope, kv_latent, rope_key, latent_gain.reshape(1, -1), cosine, sine,
        w_key, w_value, w_out, post_gain.reshape(1, -1),
    )


def tables(positions, rot_width):
    frequency = 1.0 / rope_base ** (jnp.arange(0, rot_width, 2, dtype=jnp.float32) / rot_width)
    angles = positions.astype(jnp.float32)[:, None] * frequency[None, :]
    return (jnp.cos(angles), jnp.sin(angles))


def body(
    residual,
    query_nope,
    query_rope,
    kv_latent,
    rope_key,
    latent_gain,
    w_key,
    w_value,
    w_out,
    post_gain,
    routes,
    route_weight,
    moe_gain,
    w_gate,
    w_up,
    w_down,
):
    updated = attention(
        residual, query_nope, query_rope, kv_latent, rope_key, latent_gain, w_key, w_value, w_out, post_gain
    )
    return moe(updated, routes, route_weight, moe_gain, w_gate, w_up, w_down)


def solution(mesh):
    placed = (
        P(GRP_SP_TP, None),
        P(GRP_SP, "tp"),
        P(GRP_SP, "tp"),
        P(GRP_SP, None),
        P(GRP_SP, None),
        P(),
        P(None, "tp"),
        P(None, "tp"),
        P("tp", None),
        P(),
        P(GRP_SP_TP, None),
        P(GRP_SP_TP, None),
        P(),
        P(SP, None, "tp"),
        P(SP, None, "tp"),
        P(SP, "tp", None),
    )
    return jax.shard_map(
        body, mesh=mesh, in_specs=placed, out_specs=P(GRP_SP_TP, None), check_vma=False
    )
```
